32 devices in a mesh: rep: 2 (over x), fs: 4 (over z), tp: 4 (over y, core).
Axes of the slice: x: 2, y: 2, z: 4, core: 2. Of those that a mesh axis runs over, the one named last changes fastest.
Arguments:
- tokens: bfloat16 [4096, 2048], P(('rep', 'fs', 'tp')), may hold values from -6 to 6
- mix_gain: float32 [2048], replicated, may hold values from 0.1 to 1.9
- w_query: bfloat16 [2048, 1024], P('fs', 'tp'), may hold values from -0.125 to 0.125
- w_key: bfloat16 [2048, 1024], P('fs', 'tp'), may hold values from -0.125 to 0.125
- w_value: bfloat16 [2048, 2048], P('fs', 'tp'), may hold values from -0.125 to 0.125
- w_decay_down: bfloat16 [2048, 32], replicated, may hold values from -0.125 to 0.125
- w_decay_up: bfloat16 [32, 1024], replicated, may hold values from -2 to 2
- decay_bias: float32 [1024], replicated, may hold values from -1 to 6
- decay_shift: float32 [4096, 1024], P(('rep', 'fs'), 'tp'), may hold values from -3 to 0
- head_gain: float32 [2048], replicated, may hold values from 0.1 to 1.9
- w_mix_out: bfloat16 [2048, 2048], P('tp', 'fs'), may hold values from -0.125 to 0.125
- ffn_gain: float32 [2048], replicated, may hold values from 0.1 to 1.9
- w_gate: bfloat16 [2048, 5632], P('fs', 'tp'), may hold values from -0.125 to 0.125
- w_up: bfloat16 [2048, 5632], P('fs', 'tp'), may hold values from -0.125 to 0.125
- w_down: bfloat16 [5632, 2048], P('tp', 'fs'), may hold values from -0.078125 to 0.078125
Outputs:
- layer_out: float32 [4096, 2048], P(('rep', 'fs', 'tp'))
The draws below stay inside these ranges and needn't reach their ends.
All inputs are finite; a program needn't handle non-finite values.
Results may differ from the reference program's by a relative error of at most 0.04.
Values may be sent and summed in bfloat16 or wider, within the bound.
A program may use at most 128 MiB of HBM per device.

```python
import jax
import jax.numpy as jnp
from jax import lax

D = 2048
HEADS = 8
KEY_CHANNELS = 128
DV = 256
KEY = 1024
RANK = 32
FF = 5632
BLK = 64
SEQUENCE_LENGTH = 512
TOKENS = 4096
N_TP = 4


def draw_decay_bias(key, part):
    head_key, fast_key, slow_key = jax.random.split(key, 3)
    fast_chance = 0.5
    fast_heads = jax.random.bernoulli(head_key, fast_chance, (HEADS,))
    fast_values = jax.random.uniform(fast_key, (HEADS, KEY_CHANNELS), jnp.float32, -0.5, 1.5)
    slow_values = jax.random.uniform(slow_key, (HEADS, KEY_CHANNELS), jnp.float32, 4.0, 6.0)
    return jnp.where(fast_heads[:, None], fast_values, slow_values).reshape(KEY).astype(jnp.float32)


def draw_decay_shift(key, part):
    sequence_count = TOKENS // SEQUENCE_LENGTH
    location_key, depth_key, rate_key = jax.random.split(key, 3)
    spike_locations = jax.random.randint(location_key, (sequence_count, 3), 0, SEQUENCE_LENGTH)
    spike_magnitudes = jnp.log(jax.random.uniform(depth_key, (sequence_count, 3, HEADS), jnp.float32, 0.5, 0.8))
    row_ids = jnp.arange(TOKENS)
    sequence_index = row_ids // SEQUENCE_LENGTH
    token_positions = row_ids % SEQUENCE_LENGTH
    match_flags = (token_positions[:, None] == spike_locations[sequence_index]).astype(jnp.float32)
    spike_events = jnp.einsum('fi,fit->ft', match_flags, spike_magnitudes[sequence_index])
    block_count = TOKENS // BLK
    rates = -jnp.exp(jax.random.uniform(rate_key, (block_count, KEY), jnp.float32, jnp.log(0.3), jnp.log(3.0))) / SEQUENCE_LENGTH
    decay_rate_rows = jnp.repeat(rates, BLK, axis=0)
    return (jnp.repeat(spike_events, KEY_CHANNELS, axis=1) + decay_rate_rows).astype(jnp.float32)


def shard_levels(stream_key, dims, cuts, smallest, top_value):
    level, own = 1.0, jax.random.fold_in(stream_key, 6)
    for position, parts in cuts:
        heights = jnp.exp(jax.random.uniform(jax.random.fold_in(own, position), (parts,), jnp.float32, smallest / len(cuts), top_value / len(cuts)))
        level = level * jnp.repeat(heights, dims[position] // parts).reshape([-1 if axis == position else 1 for axis in range(len(dims))])
    return level


def scatter_about(stream_key, shape, spread, bound, cuts=(), dtype=jnp.bfloat16):
    drawn = spread * jax.random.normal(stream_key, shape, jnp.float32)
    if cuts:
        drawn = drawn * shard_levels(stream_key, shape, cuts, -0.22, 0.18)
    return jnp.clip(drawn, -bound, bound).astype(dtype)


def setup_inputs(seed: int = 0) -> dict:
    streams_of = jax.random.split(jax.random.key(seed), 16)
    return {
        "tokens": scatter_about(streams_of[0], (TOKENS, D), 1.0, 6.0, ((0, 32),)),
        "mix_gain": jnp.clip(1.0 + 0.18 * jax.random.normal(streams_of[1], (D,), jnp.float32), 0.1, 1.9),
        "w_query": scatter_about(streams_of[2], (D, KEY), D ** -0.5, 0.125, ((0, 4), (1, 4))),
        "w_key": scatter_about(streams_of[3], (D, KEY), D ** -0.5, 0.125, ((0, 4), (1, 4))),
        "w_value": scatter_about(streams_of[4], (D, D), D ** -0.5, 0.125, ((0, 4), (1, 4))),
        "w_decay_down": scatter_about(streams_of[5], (D, RANK), D ** -0.5, 0.125),
        "w_decay_up": scatter_about(streams_of[6], (RANK, KEY), (RANK // 4) ** -0.5, 2.0),
        "decay_bias": draw_decay_bias(jax.random.fold_in(streams_of[15], 71), 0),
        "decay_shift": draw_decay_shift(jax.random.fold_in(streams_of[15], 71), 0),
        "head_gain": jnp.clip(1.0 + 0.18 * jax.random.normal(streams_of[9], (D,), jnp.float32), 0.1, 1.9),
        "w_mix_out": scatter_about(streams_of[10], (D, D), D ** -0.5, 0.125, ((0, 4), (1, 4))),
        "ffn_gain": jnp.clip(1.0 + 0.18 * jax.random.normal(streams_of[11], (D,), jnp.float32), 0.1, 1.9),
        "w_gate": scatter_about(streams_of[12], (D, FF), D ** -0.5, 0.125, ((0, 4), (1, 4))),
        "w_up": scatter_about(streams_of[13], (D, FF), D ** -0.5, 0.125, ((0, 4), (1, 4))),
        "w_down": scatter_about(streams_of[14], (FF, D), FF ** -0.5, 0.078125, ((0, 4), (1, 4))),
    }


EPS = 1e-06
TAU = 16.0

def rms_norm(values, gain):
    return values * lax.rsqrt(lax.optimization_barrier(jnp.mean(values * values, axis=-1, keepdims=True)) + EPS) * gain

def recurrence(query_proj, key_proj, value_proj, log_decay):
    blocks = SEQUENCE_LENGTH // BLK
    queries = query_proj.astype(jnp.float32).reshape(blocks, BLK, HEADS, KEY_CHANNELS) * KEY_CHANNELS ** (-0.5)
    keys = key_proj.astype(jnp.float32).reshape(blocks, BLK, HEADS, KEY_CHANNELS)
    values = value_proj.astype(jnp.float32).reshape(blocks, BLK, HEADS, DV)
    decays = log_decay.reshape(blocks, BLK, HEADS, KEY_CHANNELS)
    cumul = jnp.cumsum(decays, axis=1)
    totals = cumul[:, -1]
    weighted = keys * jnp.exp(totals[:, None] - cumul)
    updates = jnp.einsum('bchd,bche->bhde', weighted, values, precision=lax.Precision.HIGHEST)

    def advance(state, inputs):
        total, update = inputs
        new_state = jnp.exp(total)[..., None] * state + update
        return (new_state, state)
    _, previous = lax.scan(advance, jnp.zeros((HEADS, KEY_CHANNELS, DV), jnp.float32), (totals, updates))
    q_decayed = queries * jnp.exp(cumul)
    k_decayed = keys * jnp.exp(-cumul)
    scores = jnp.einsum('bchd,bshd->bhcs', q_decayed, k_decayed, precision=lax.Precision.HIGHEST)
    causal = (jnp.arange(BLK)[:, None] >= jnp.arange(BLK)[None, :]).astype(jnp.float32)
    scores = scores * causal
    inner = jnp.einsum('bhcs,bshe->bche', scores, values, precision=lax.Precision.HIGHEST)
    carried = jnp.einsum('bchd,bhde->bche', q_decayed, previous, precision=lax.Precision.HIGHEST)
    return (inner + carried).reshape(SEQUENCE_LENGTH, HEADS, DV)

def reference(tokens, mix_gain, w_query, w_key, w_value, w_decay_down, w_decay_up, decay_bias, decay_shift, head_gain, w_mix_out, ffn_gain, w_gate, w_up, w_down):
    sequence_count = TOKENS // SEQUENCE_LENGTH
    out_groups = w_mix_out.astype(jnp.float32).reshape(N_TP, D // N_TP, D)
    down_groups = w_down.astype(jnp.float32).reshape(N_TP, FF // N_TP, D)

    def layer(inputs):
        seq_tokens, seq_shift = inputs
        source = seq_tokens.astype(jnp.float32)
        normed = rms_norm(source, mix_gain).astype(jnp.bfloat16)
        query_proj = jnp.dot(normed, w_query, preferred_element_type=jnp.float32).astype(jnp.bfloat16)
        key_proj = jnp.dot(normed, w_key, preferred_element_type=jnp.float32).astype(jnp.bfloat16)
        value_proj = jnp.dot(normed, w_value, preferred_element_type=jnp.float32).astype(jnp.bfloat16)
        low_rank = jnp.dot(normed, w_decay_down, preferred_element_type=jnp.float32).astype(jnp.bfloat16)
        pre_decay = jnp.dot(low_rank, w_decay_up, preferred_element_type=jnp.float32) + decay_bias
        log_decay = jax.nn.log_sigmoid(pre_decay) / TAU + seq_shift
        head_out = recurrence(query_proj, key_proj, value_proj, log_decay)
        gated = rms_norm(head_out, head_gain.reshape(HEADS, DV)).astype(jnp.bfloat16)
        gated = gated.reshape(SEQUENCE_LENGTH, N_TP, D // N_TP).astype(jnp.float32)
        partials = jnp.einsum('lgc,gcd->gld', gated, out_groups).astype(jnp.bfloat16)
        hidden = source + lax.optimization_barrier(jnp.sum(partials.astype(jnp.float32), axis=0))
        normed_ffn = rms_norm(hidden, ffn_gain).astype(jnp.bfloat16)
        gate_proj = jnp.dot(normed_ffn, w_gate, preferred_element_type=jnp.float32)
        up_proj = jnp.dot(normed_ffn, w_up, preferred_element_type=jnp.float32)
        activated = (jax.nn.silu(gate_proj) * up_proj).astype(jnp.bfloat16)
        activated = activated.reshape(SEQUENCE_LENGTH, N_TP, FF // N_TP).astype(jnp.float32)
        ffn_parts = jnp.einsum('lgc,gcd->gld', activated, down_groups).astype(jnp.bfloat16)
        return hidden + lax.optimization_barrier(jnp.sum(ffn_parts.astype(jnp.float32), axis=0))
    result = lax.map(layer, (tokens.reshape(sequence_count, SEQUENCE_LENGTH, D), decay_shift.reshape(sequence_count, SEQUENCE_LENGTH, KEY)))
    return result.reshape(TOKENS, D)
```

```python
import jax
import jax.numpy as jnp
from jax import lax
from jax.sharding import PartitionSpec as P

KEY_CHANNELS = 128
DV = 256
BLK = 64


EPS = 1e-06
TAU = 16.0


def rms_norm(values, gain):
    return values * lax.rsqrt(jnp.mean(values * values, axis=-1, keepdims=True) + EPS) * gain


def recurrence(query_proj, key_proj, value_proj, log_decay, head_count):
    seq_rows = query_proj.shape[0]
    blocks = seq_rows // BLK
    exact = lax.Precision.HIGHEST
    queries = query_proj.astype(jnp.float32).reshape(
        blocks, BLK, head_count, KEY_CHANNELS
    ) * KEY_CHANNELS ** (-0.5)
    keys = key_proj.astype(jnp.float32).reshape(blocks, BLK, head_count, KEY_CHANNELS)
    values = value_proj.astype(jnp.float32).reshape(blocks, BLK, head_count, DV)
    decays = log_decay.reshape(blocks, BLK, head_count, KEY_CHANNELS)
    lower = (jnp.arange(BLK)[:, None] >= jnp.arange(BLK)[None, :]).astype(jnp.float32)
    cumul = jnp.einsum("cs,bshd->bchd", lower, decays, precision=exact)
    totals = cumul[:, -1]
    weighted = keys * jnp.exp(totals[:, None] - cumul)
    updates = jnp.einsum("bchd,bche->bhde", weighted, values, precision=exact)
    state = jnp.zeros_like(updates[0])
    previous = []
    for block in range(blocks):
        previous.append(state)
        state = jnp.exp(totals[block])[..., None] * state + updates[block]
    previous = jnp.stack(previous)
    q_decayed = queries * jnp.exp(cumul)
    k_decayed = keys * jnp.exp(-cumul)
    scores = jnp.einsum("bchd,bshd->bhcs", q_decayed, k_decayed, precision=exact)
    scores = scores * lower
    inner = jnp.einsum("bhcs,bshe->bche", scores, values, precision=exact)
    carried = jnp.einsum("bchd,bhde->bche", q_decayed, previous, precision=exact)
    return (inner + carried).reshape(seq_rows, head_count, DV)


def shift(values, axis, distance):
    count = lax.axis_size(axis)
    return lax.ppermute(values, axis, [(i, (i + distance) % count) for i in range(count)])


def swap_core(values):
    return lax.ppermute(values, "tp", [(i, i ^ 1) for i in range(lax.axis_size("tp"))])


def gather_rows(block):
    count = lax.axis_size("tp")
    index = lax.axis_index("tp")
    chips, core, chip = count // 2, index % 2, index // 2
    rows = block.shape[0]
    mine = [block] + [shift(block, "tp", 2 * k) for k in range(1, chips)]
    whole = jnp.zeros((count * rows,) + block.shape[1:], block.dtype)
    for k, piece in enumerate(mine):
        source = (chip - k) % chips
        theirs = swap_core(piece)
        whole = lax.dynamic_update_slice_in_dim(whole, piece, (2 * source + core) * rows, 0)
        whole = lax.dynamic_update_slice_in_dim(whole, theirs, (2 * source + 1 - core) * rows, 0)
    return whole


def scatter_sum(partial):
    count = lax.axis_size("tp")
    index = lax.axis_index("tp")
    chips, core, chip = count // 2, index % 2, index // 2
    rows = partial.shape[0] // count
    blocks = partial.astype(jnp.bfloat16).reshape(chips, 2, rows, partial.shape[1])
    away = lax.dynamic_index_in_dim(blocks, 1 - core, 1, keepdims=False)
    kept = lax.dynamic_index_in_dim(blocks, core, 1, keepdims=False).astype(jnp.float32)
    pair = kept + swap_core(away).astype(jnp.float32)
    rounded = pair.astype(jnp.bfloat16)
    total = lax.dynamic_index_in_dim(pair, chip, 0, keepdims=False)
    for k in range(1, chips):
        outgoing = lax.dynamic_index_in_dim(rounded, (chip + k) % chips, 0, keepdims=False)
        total = total + shift(outgoing, "tp", 2 * k).astype(jnp.float32)
    return total


def row_parts(weight):
    reps = lax.axis_size("rep")
    share = weight.shape[0] // reps
    own = lax.dynamic_slice_in_dim(weight, lax.axis_index("rep") * share, share, 0)
    own = lax.all_gather(own, "fs", axis=0, tiled=True)
    return [own] + [shift(own, "rep", k) for k in range(1, reps)]


def column_parts(weight):
    reps = lax.axis_size("rep")
    share = weight.shape[1] // reps
    own = lax.dynamic_slice_in_dim(weight, lax.axis_index("rep") * share, share, 1)
    own = lax.all_gather(own, "fs", axis=0, tiled=False)
    return [own] + [shift(own, "rep", k) for k in range(1, reps)]


def input_parts(values):
    reps, groups = lax.axis_size("rep"), lax.axis_size("fs")
    share = values.shape[1] // (reps * groups)
    layouts = [
        jnp.concatenate(
            [
                values[:, (g * reps + j) * share : (g * reps + j + 1) * share]
                for g in range(groups)
            ],
            axis=1,
        )
        for j in range(reps)
    ]
    index = lax.axis_index("rep")
    return [
        lax.select_n(jnp.full((), (index - k) % reps, jnp.int32), *layouts) if reps > 2
        else (jnp.where((index - k) % reps == 0, layouts[0], layouts[-1]))
        for k in range(reps)
    ]


def dots(inputs, weights):
    total = jnp.dot(inputs[0], weights[0], preferred_element_type=jnp.float32)
    for left, right in zip(inputs[1:], weights[1:]):
        total = total + jnp.dot(left, right, preferred_element_type=jnp.float32)
    return total


def project_out(values, weights):
    reps = lax.axis_size("rep")
    index = lax.axis_index("rep")
    sums = []
    for weight in weights:
        partial = jnp.concatenate(
            [
                jnp.dot(values, weight[g], preferred_element_type=jnp.float32)
                for g in range(weight.shape[0])
            ],
            axis=1,
        )
        sums.append(scatter_sum(partial))
    share = weights[0].shape[2]
    ordered = []
    for j in range(reps):
        if reps == 2:
            ordered.append(jnp.where(index == j, sums[0], sums[1]))
        else:
            ordered.append(lax.select_n((index - j) % reps, *sums))
    pieces = []
    for g in range(weights[0].shape[0]):
        for j in range(reps):
            pieces.append(ordered[j][:, g * share : (g + 1) * share])
    return jnp.concatenate(pieces, axis=1)


def per_device(
    tokens,
    mix_gain,
    w_query,
    w_key,
    w_value,
    w_decay_down,
    w_decay_up,
    decay_bias,
    decay_shift,
    head_gain,
    w_mix_out,
    ffn_gain,
    w_gate,
    w_up,
    w_down,
):
    tp_index = lax.axis_index("tp")
    key_cols = w_query.shape[1]
    value_cols = w_value.shape[1]
    heads_dev = key_cols // KEY_CHANNELS
    own_tokens = tokens.astype(jnp.float32)
    qkv_weights = row_parts(jnp.concatenate([w_query, w_key, w_value], axis=1))
    out_weights = column_parts(w_mix_out)
    gate_weights = row_parts(w_gate)
    up_weights = row_parts(w_up)
    down_weights = column_parts(w_down)
    normed = gather_rows(rms_norm(own_tokens, mix_gain).astype(jnp.bfloat16))
    seq_rows = normed.shape[0]
    low_rank = jnp.dot(normed, w_decay_down, preferred_element_type=jnp.float32).astype(
        jnp.bfloat16
    )
    up_columns = lax.dynamic_slice_in_dim(w_decay_up, tp_index * key_cols, key_cols, 1)
    bias_columns = lax.dynamic_slice_in_dim(decay_bias, tp_index * key_cols, key_cols, 0)
    pre_decay = jnp.dot(low_rank, up_columns, preferred_element_type=jnp.float32) + bias_columns
    log_decay = jax.nn.log_sigmoid(pre_decay) / TAU + decay_shift
    projected = dots(input_parts(normed), qkv_weights).astype(jnp.bfloat16)
    query_proj = projected[:, :key_cols]
    key_proj = projected[:, key_cols : 2 * key_cols]
    value_proj = projected[:, 2 * key_cols :]
    head_out = recurrence(query_proj, key_proj, value_proj, log_decay, heads_dev)
    gain_columns = lax.dynamic_slice_in_dim(head_gain, tp_index * value_cols, value_cols, 0)
    gated = rms_norm(head_out, gain_columns.reshape(heads_dev, DV)).astype(jnp.bfloat16)
    gated = gated.reshape(seq_rows, value_cols)
    hidden = own_tokens + project_out(gated, out_weights)
    normed_ffn = gather_rows(rms_norm(hidden, ffn_gain).astype(jnp.bfloat16))
    ffn_inputs = input_parts(normed_ffn)
    gate_proj = dots(ffn_inputs, gate_weights)
    up_proj = dots(ffn_inputs, up_weights)
    activated = (jax.nn.silu(gate_proj) * up_proj).astype(jnp.bfloat16)
    return hidden + project_out(activated, down_weights)


def solution(mesh):
    return jax.shard_map(
        per_device,
        mesh=mesh,
        in_specs=(
            P(("rep", "fs", "tp"), None),
            P(),
            P("fs", "tp"),
            P("fs", "tp"),
            P("fs", "tp"),
            P(),
            P(),
            P(),
            P(("rep", "fs"), "tp"),
            P(),
            P("tp", "fs"),
            P(),
            P("fs", "tp"),
            P("fs", "tp"),
            P("tp", "fs"),
        ),
        out_specs=P(("rep", "fs", "tp"), None),
        check_vma=False,
    )
```
